32 devices in a mesh: tp: 8 (over z, y), dp: 4 (over x, core).
Axes of the slice: x: 2, y: 2, z: 4, core: 2. Of those that a mesh axis runs over, the one named last changes fastest.
Arguments:
- tokens: bfloat16 [64, 4096], P('tp', 'dp'), may hold values from -30 to 30
- lengths: int32 [64], P('dp'), may hold values from 1 to 2048, 16384 in all
- states: float32 [2, 64, 2048, 128], P(None, 'dp', 'tp'), may hold values from -0.8 to 0.8
- norm_gain: bfloat16 [2, 4096], P(None, 'dp'), may hold values from 0.099609375 to 1.8984375
- w_query: bfloat16 [2, 4096, 2048], P(None, 'dp', 'tp'), may hold values from -0.09375 to 0.09375
- w_key: bfloat16 [2, 4096, 2048], P(None, 'dp', 'tp'), may hold values from -0.09375 to 0.09375
- w_value: bfloat16 [2, 4096, 2048], P(None, 'dp', 'tp'), may hold values from -0.09375 to 0.09375
- w_gate: bfloat16 [2, 4096, 2048], P(None, 'dp', 'tp'), may hold values from -0.09375 to 0.09375
- head_gain: bfloat16 [2, 2048], P(None, 'tp'), may hold values from 0.099609375 to 1.8984375
- w_out: bfloat16 [2, 2048, 4096], P(None, 'tp', 'dp'), may hold values from -0.125 to 0.125
Outputs:
- hidden_out: bfloat16 [64, 4096], P('tp', 'dp')
- new_states: float32 [2, 64, 2048, 128], P(None, 'dp', 'tp')
The draws below stay inside these ranges and needn't reach their ends.
All inputs are finite; a program needn't handle non-finite values. No bound on the sum of `lengths` on one device may be relied on, other than what follows from the above.
Results may differ from the reference program's by a relative error of at most 0.012.
Values may be sent and summed in bfloat16 or wider, within the bound.
A program may use at most 64 MiB of HBM per device.

```python
import math
import jax
import jax.numpy as jnp
import numpy as np
from jax import lax

D = 4096
HEADS = 16
DK = 128
LAYERS = 2
SEQS = 64


def draw_tokens(key, part):
    key_base, key_rough = jax.random.split(jax.random.fold_in(key, 11), 2)
    base_draw = jax.random.normal(key_base, (SEQS, D), jnp.float32)
    column = jnp.arange(D, dtype=jnp.float32) / (D - 1)
    rough = jax.random.uniform(key_rough, (D,), jnp.float32, 0.5, 1.5)
    column_scale = jnp.exp(math.log(3.0) * column) * rough
    result = base_draw * column_scale[None, :]
    return jnp.clip(result, -30.0, 30.0).astype(jnp.bfloat16)


def block_scale(key, shape, pieces, smallest, high):
    level = 1.0
    for axis_at, blocks in pieces:
        steps = jax.random.uniform(jax.random.fold_in(jax.random.fold_in(key, 6), axis_at), (blocks,), jnp.float32, smallest / len(pieces), high / len(pieces))
        level = level * jnp.repeat(jnp.exp(steps), shape[axis_at] // blocks).reshape((-1,) + (1,) * (len(shape) - 1 - axis_at))
    return level


def profile(number_of, total, limit, skew):
    loads = [(1 << 20) // math.isqrt(standing ** skew) + 1 for standing in range(2, number_of + 1)]
    spare, counts = total - limit - (number_of - 1), [1] * (number_of - 1)
    while spare > 0:
        candidates = [i for i in range(number_of - 1) if counts[i] < limit]
        mass, remaining = sum([loads[i] for i in candidates]), spare
        for i in candidates:
            addition = min(limit - counts[i], max(1, remaining * loads[i] // mass), spare)
            counts[i] = counts[i] + addition
            spare = spare - addition
    return np.array([limit] + counts)


def uneven(key, count, total, most, slope):
    if count == 2:
        one = jax.random.randint(key, (), max(1, total - most), min(most, total - 1) + 1)
        return jnp.stack([one, total - one])
    tallies = jnp.asarray(profile(count, total, most, slope), jnp.int32)
    couples = (count - 1) // 2
    source_of, sink = tallies[1:1 + 2 * couples:2], tallies[2:2 + 2 * couples:2]
    slack = jnp.minimum(source_of - 1, most - sink)
    moved = jax.random.randint(jax.random.fold_in(key, 1), (couples,), 0, 1 << 20) % (slack + 1)
    tallies = tallies.at[1:1 + 2 * couples:2].set(source_of - moved).at[2:2 + 2 * couples:2].set(sink + moved)
    return tallies[jax.random.permutation(jax.random.fold_in(key, 2), count)]


def scatter_about(rng, extent, width, reach, shards=(), kind=jnp.bfloat16):
    values = jax.random.normal(rng, extent, jnp.float32) * width
    if len(shards) > 0:
        values = block_scale(rng, extent, shards, -0.22, 0.18) * values
    return jnp.clip(values, min=-reach, max=reach).astype(kind)


def setup_inputs(seed: int = 0) -> dict:
    key_of = jax.random.split(jax.random.key(seed), 11)
    return {
        "tokens": draw_tokens(jax.random.fold_in(key_of[10], 71), 0),
        "lengths": uneven(key_of[1], SEQS, SEQS * 256, 2048, 2).astype(jnp.int32),
        "states": scatter_about(key_of[2], (LAYERS, SEQS, HEADS * DK, DK), 0.1, 0.8, ((1, 4), (2, 8)), jnp.float32),
        "norm_gain": jnp.clip(1.0 + 0.18 * jax.random.normal(key_of[3], (LAYERS, D), jnp.float32), 0.099609375, 1.8984375).astype(jnp.bfloat16),
        "w_query": scatter_about(key_of[4], (LAYERS, D, HEADS * DK), D ** -0.5, 0.09375, ((1, 4), (2, 8))),
        "w_key": scatter_about(key_of[5], (LAYERS, D, HEADS * DK), D ** -0.5, 0.09375, ((1, 4), (2, 8))),
        "w_value": scatter_about(key_of[6], (LAYERS, D, HEADS * DK), D ** -0.5, 0.09375, ((1, 4), (2, 8))),
        "w_gate": scatter_about(key_of[7], (LAYERS, D, HEADS * DK), D ** -0.5, 0.09375, ((1, 4), (2, 8))),
        "head_gain": jnp.clip(1.0 + 0.18 * jax.random.normal(key_of[8], (LAYERS, HEADS * DK), jnp.float32), 0.099609375, 1.8984375).astype(jnp.bfloat16),
        "w_out": scatter_about(key_of[9], (LAYERS, HEADS * DK, D), (HEADS * DK) ** -0.5, 0.125, ((1, 8), (2, 4))),
    }


norm_eps = 1e-06
group_eps = 1e-05
rotary_base = 10000.0

def rotate(values, positions):
    half_size = values.shape[-1] // 2
    inverse = rotary_base ** (-jnp.arange(half_size, dtype=jnp.float32) / half_size)
    angles = positions.astype(jnp.float32)[:, None] * inverse[None, :]
    cosine = jnp.cos(angles)[:, None, :]
    sine_v = jnp.sin(angles)[:, None, :]
    first_part = values[..., :half_size]
    second = values[..., half_size:]
    return jnp.concatenate([first_part * cosine - second * sine_v, first_part * sine_v + second * cosine], axis=-1)

def decays(head_ids):
    return 1.0 - jnp.exp2(-1.0 - 9.0 * head_ids.astype(jnp.float32) / (HEADS - 1))

def reference(tokens, lengths, states, norm_gain, w_query, w_key, w_value, w_gate, head_gain, w_out):
    batch_size = tokens.shape[0]
    full_width = HEADS * DK
    gammas = decays(jnp.arange(HEADS, dtype=jnp.int32))
    hidden_x = tokens
    outputs = []
    for layer_id in range(LAYERS):
        xfloat = hidden_x.astype(jnp.float32)
        row_scale = lax.rsqrt(lax.optimization_barrier(jnp.sum(xfloat * xfloat, axis=1)) / D + norm_eps)
        normed = (xfloat * norm_gain[layer_id].astype(jnp.float32)).astype(jnp.bfloat16)

        def project(weight):
            product = jnp.dot(normed, weight[layer_id], preferred_element_type=jnp.float32)
            return (product * row_scale[:, None]).astype(jnp.bfloat16)
        query_rows = rotate(project(w_query).astype(jnp.float32).reshape(batch_size, HEADS, DK), lengths)
        key_rows = rotate(project(w_key).astype(jnp.float32).reshape(batch_size, HEADS, DK), lengths) * DK ** (-0.5)
        values_f = project(w_value).astype(jnp.float32).reshape(batch_size, HEADS, DK)
        gate_rows = project(w_gate).astype(jnp.float32)
        prior_state = states[layer_id].reshape(batch_size, HEADS, DK, DK)
        updated = gammas[None, :, None, None] * prior_state + jnp.einsum('bhd,bhv->bhvd', key_rows, values_f)
        readout = jnp.einsum('bhd,bhvd->bhv', query_rows, updated)
        mean_v = lax.optimization_barrier(jnp.mean(readout, axis=-1, keepdims=True))
        square = lax.optimization_barrier(jnp.mean(readout * readout, axis=-1, keepdims=True))
        grouped = ((readout - mean_v) * lax.rsqrt(square - mean_v * mean_v + group_eps)).reshape(batch_size, full_width)
        grouped = grouped * head_gain[layer_id].astype(jnp.float32)
        gated_rows = (jax.nn.silu(gate_rows) * grouped).astype(jnp.bfloat16)
        hidden_x = (xfloat + jnp.dot(gated_rows, w_out[layer_id], preferred_element_type=jnp.float32)).astype(jnp.bfloat16)
        outputs.append(updated.reshape(batch_size, full_width, DK))
    return (hidden_x, jnp.stack(outputs))
```

```python
import contextlib
import math

import jax
import jax.numpy as jnp
from jax import lax
from jax.experimental import pallas as pl
from jax.experimental.pallas import tpu as pltpu
from jax.sharding import PartitionSpec as P

D = 4096
HEADS = 16
DK = 128
LAYERS = 2


norm_eps = 1e-06
group_eps = 1e-05
rotary_base = 10000.0


def partner_2(value, axis, apart):
    mask = 2**apart
    pairs = [(source, source ^ mask) for source in range(lax.axis_size(axis))]
    return lax.ppermute(value, axis, pairs)


def rotate(values, positions):
    half_size = values.shape[-1] // 2
    inverse = rotary_base ** (-jnp.arange(half_size, dtype=jnp.float32) / half_size)
    angles = positions.astype(jnp.float32)[:, None] * inverse[None, :]
    cosine = jnp.cos(angles)[:, None, :]
    sine_v = jnp.sin(angles)[:, None, :]
    first_part = values[..., :half_size]
    second = values[..., half_size:]
    return jnp.concatenate(
        [first_part * cosine - second * sine_v, first_part * sine_v + second * cosine], axis=-1
    )


def decays(head_ids):
    return 1.0 - jnp.exp2(-1.0 - 9.0 * head_ids.astype(jnp.float32) / (HEADS - 1))


def split_head_body(tokens, lengths, states, norm_gain, w_query, w_key, w_value, w_gate, head_gain, w_out):
    tp_index = lax.axis_index("tp")
    dp_index = lax.axis_index("dp")
    tp_count = lax.axis_size("tp")
    columns = w_query.shape[2]
    pieces = max(DK // columns, 1)
    levels = pieces.bit_length() - 1
    local_heads = max(columns // DK, 1)
    value_cols = columns // local_heads
    head_ids = tp_index * columns // DK + jnp.arange(local_heads, dtype=jnp.int32)
    gammas = decays(head_ids)
    hidden_x = tokens
    outputs = []
    for layer_id in range(LAYERS):
        prior_state = states[layer_id]
        row_total = prior_state.shape[0]
        local_rows = hidden_x.shape[0]
        x_float = hidden_x.astype(jnp.float32)
        feature_gain = norm_gain[layer_id].astype(jnp.float32)
        weights = jnp.concatenate(
            [w_query[layer_id], w_key[layer_id], w_value[layer_id], w_gate[layer_id]], axis=1
        )
        gathered = lax.all_gather(hidden_x, "tp", axis=0, tiled=True)
        gathered_f = gathered.astype(jnp.float32)
        normed = (gathered_f * feature_gain).astype(jnp.bfloat16)
        partial_value = jnp.dot(normed, weights, preferred_element_type=jnp.float32)
        squares_full = jnp.zeros((local_rows * tp_count,), jnp.float32)
        squares_full = lax.dynamic_update_slice_in_dim(
            squares_full, jnp.sum(x_float * x_float, axis=1), tp_index * local_rows, 0
        )
        all_squares = lax.psum(squares_full, ("tp", "dp"))
        summed = lax.psum_scatter(partial_value, "dp", scatter_dimension=0, tiled=True)
        own_squares = lax.dynamic_slice_in_dim(all_squares, dp_index * row_total, row_total, 0)
        row_scale = lax.rsqrt(own_squares / D + norm_eps)
        projected = (summed * row_scale[:, None]).astype(jnp.bfloat16)
        query_rows = projected[:, :columns]
        key_rows = projected[:, columns : 2 * columns]
        value_rows = projected[:, 2 * columns : 3 * columns]
        gate_rows = projected[:, 3 * columns :]
        stacked = jnp.stack([query_rows, key_rows])
        for join_level_id in range(levels):
            partner = partner_2(stacked, "tp", join_level_id)
            upper_bit = tp_index // 2**join_level_id % 2
            stacked = jnp.where(
                upper_bit == 1,
                jnp.concatenate([partner, stacked], axis=-1),
                jnp.concatenate([stacked, partner], axis=-1),
            )
        query_f = rotate(
            stacked[0].astype(jnp.float32).reshape(row_total, local_heads, DK), lengths
        )
        key_f = rotate(
            stacked[1].astype(jnp.float32).reshape(row_total, local_heads, DK), lengths
        ) * DK ** (-0.5)
        values_f = value_rows.astype(jnp.float32).reshape(row_total, local_heads, value_cols)
        state_view = prior_state.reshape(row_total, local_heads, value_cols, DK)
        updated = gammas[None, :, None, None] * state_view + jnp.einsum(
            "shd,shv->shvd", key_f, values_f
        )
        readout = jnp.einsum("shd,shvd->shv", query_f, updated)
        head_stats = jnp.stack([jnp.sum(readout, axis=-1), jnp.sum(readout * readout, axis=-1)])
        for level_id in range(levels):
            head_stats = head_stats + partner_2(head_stats, "tp", level_id)
        mean_v = head_stats[0][..., None] / DK
        square = head_stats[1][..., None] / DK
        grouped = ((readout - mean_v) * lax.rsqrt(square - mean_v * mean_v + group_eps)).reshape(
            row_total, columns
        )
        grouped = grouped * head_gain[layer_id].astype(jnp.float32)
        gated_rows = (jax.nn.silu(gate_rows.astype(jnp.float32)) * grouped).astype(jnp.bfloat16)
        out_weight = w_out[layer_id]
        whole_weight = lax.all_gather(out_weight, "tp", axis=0, tiled=True)
        every_row = lax.all_gather(gated_rows, "dp", axis=0, tiled=True)
        owned_rows = lax.all_to_all(every_row, "tp", split_axis=0, concat_axis=1, tiled=True)
        branch = jnp.dot(owned_rows, whole_weight, preferred_element_type=jnp.float32)
        hidden_x, updated = (
            (x_float + branch).astype(jnp.bfloat16),
            updated.reshape(row_total, columns, DK),
        )
        outputs.append(updated)
    return (hidden_x, jnp.stack(outputs))


MESH = pl.DeviceIdType.MESH
KINDS = 4
GROUP = 2
GROUPS = KINDS // GROUP
OUT_PIECES = 4
TRACED = False


def stage(name):
    return jax.named_scope(name) if TRACED else contextlib.nullcontext()


def decay_row(columns):
    channel = lax.axis_index("tp") * columns + lax.broadcasted_iota(jnp.int32, (1, columns), 1)
    head = (channel // DK).astype(jnp.float32)
    return 1.0 - jnp.exp((-1.0 - 9.0 * head / (HEADS - 1)) * math.log(2.0))


def flipped(index, mask):
    for bit in range(mask.bit_length()):
        if mask >> bit & 1:
            index = index + (1 - index // 2**bit % 2 * 2) * 2**bit
    return index


def peers_of(index, count):
    if count & (count - 1):
        return [lax.rem(index + o, count) for o in range(count)]
    return [flipped(index, mask) for mask in range(count)]


def await_bytes(ref, sem):
    pltpu.make_async_copy(ref, ref, sem).wait()


def step_kernel(
    tokens,
    lengths,
    norm_gain,
    head_gain,
    states,
    w_query,
    w_key,
    w_value,
    w_gate,
    w_out,
    hidden,
    new_states,
    length_in,
    norm_in,
    head_in,
    state_in,
    state_t,
    w_in,
    w_back,
    gathered,
    part,
    part_in,
    sq,
    sq_in,
    gated,
    branch,
    branch_in,
    fresh,
    small_sem,
    w_sem,
    state_sem,
    back_sem,
    send_sem,
    x_recv,
    p_recv,
    q_recv,
    g_recv,
    b_recv,
):
    tp, dp = lax.axis_index("tp"), lax.axis_index("dp")
    tpn, dpn = lax.axis_size("tp"), lax.axis_size("dp")
    rows, features = tokens.shape
    seqs, columns = new_states.shape[1:3]
    heads = columns // DK
    total = rows * tpn

    barrier = pltpu.get_barrier_semaphore()
    tp_peers, dp_peers = peers_of(tp, tpn), peers_of(dp, dpn)
    for o in range(1, tpn):
        pl.semaphore_signal(barrier, inc=1, device_id=(tp_peers[o], dp), device_id_type=MESH)
    for o in range(1, dpn):
        pl.semaphore_signal(barrier, inc=1, device_id=(tp, dp_peers[o]), device_id_type=MESH)

    def load(src, dst, sem):
        copy = pltpu.make_async_copy(src, dst, sem)
        copy.start()
        return copy

    got_x = load(tokens, gathered.at[tp], small_sem.at[0])
    got_small = [
        load(lengths, length_in, small_sem.at[1]),
        load(norm_gain, norm_in, small_sem.at[2]),
        load(head_gain, head_in, small_sem.at[3]),
    ]
    for copy in [got_x, *got_small]:
        copy.wait()
    got_state, got_back = [], []
    for layer in range(LAYERS):
        for j, w in enumerate((w_query, w_key, w_value, w_gate)):
            load(w.at[layer], w_in.at[layer, j], w_sem.at[layer])
        got_state.append(load(states.at[layer], state_in.at[layer], state_sem.at[layer]))
        got_back.append(load(w_out.at[layer], w_back.at[layer], back_sem.at[layer]))

    half = DK // 2
    lane = lax.broadcasted_iota(jnp.int32, (seqs, DK), 1)
    row = lax.broadcasted_iota(jnp.int32, (seqs, DK), 0)
    position = jnp.zeros((seqs, DK), jnp.float32)
    for s in range(seqs):
        position = jnp.where(row == s, length_in[s].astype(jnp.float32), position)
    inverse = jnp.exp((lane % half).astype(jnp.float32) * (-math.log(rotary_base) / half))
    angle = position * inverse
    cosine = jnp.cos(angle)
    sine = jnp.sin(angle)
    sine = jnp.where(lane < half, -sine, sine)
    gamma = decay_row(columns)

    def decay_of(h):
        return gamma[:, h * DK : h * DK + 1]

    with stage("bar_wait"):
        pl.semaphore_wait(barrier, tpn + dpn - 2)

    def send(src, dst, kind, recv_sem, where):
        pltpu.make_async_remote_copy(
            src_ref=src,
            dst_ref=dst,
            send_sem=send_sem.at[kind],
            recv_sem=recv_sem,
            device_id=where,
            device_id_type=MESH,
        ).start()

    tp_order = sorted(range(1, tpn), key=lambda o: (-o.bit_count(), -o))

    def spread_x(layer, src):
        for o in tp_order:
            send(src, gathered.at[layer * tpn + tp], 0, x_recv.at[layer], (tp_peers[o], dp))

    def turn_state(layer):
        got_state[layer].wait()
        for s in range(seqs):
            block = jnp.transpose(state_in[layer, s])
            state_t[layer, s * DK : (s + 1) * DK] = (block * gamma).astype(jnp.bfloat16)

    spread_x(0, gathered.at[tp])
    x_own = gathered[pl.ds(tp, 1)][0].astype(jnp.float32)
    with stage("turn0"):
        turn_state(0)
    for layer in range(LAYERS):
        first = layer * tpn
        await_bytes(w_in.at[layer], w_sem.at[layer])
        with stage(f"L{layer}_wait_x"):
            await_bytes(gathered.at[pl.ds(first, tpn - 1)], x_recv.at[layer])
        with stage(f"L{layer}_sq"):
            x_all = gathered[first : first + tpn].astype(jnp.float32).reshape(total, features)
            squares = x_all[:, :DK] * x_all[:, :DK]
            for at in range(DK, features, DK):
                squares = squares + x_all[:, at : at + DK] * x_all[:, at : at + DK]
            sq[layer * dpn : (layer + 1) * dpn] = squares.reshape(dpn, seqs, DK)
            for o in reversed(range(1, dpn)):
                send(
                    sq.at[layer * dpn + dp_peers[o]],
                    sq_in.at[layer, o - 1],
                    1,
                    q_recv.at[layer],
                    (tp, dp_peers[o]),
                )
            normed = (x_all * norm_in[layer : layer + 1, :].astype(jnp.float32)).astype(jnp.bfloat16)
        for group in range(GROUPS):
            slot = (layer * GROUPS + group) * dpn
            with stage(f"L{layer}_dots{group}"):
                for i in range(GROUP):
                    product = jnp.dot(
                        normed, w_in[layer, group * GROUP + i], preferred_element_type=jnp.float32
                    )
                    part[slot : slot + dpn, i] = product.astype(jnp.bfloat16).reshape(dpn, seqs, columns)
                for o in reversed(range(1, dpn)):
                    send(
                        part.at[slot + dp_peers[o]],
                        part_in.at[layer * GROUPS + group, o - 1],
                        2,
                        p_recv.at[layer * GROUPS + group],
                        (tp, dp_peers[o]),
                    )
        with stage(f"L{layer}_wait_sq"):
            await_bytes(sq_in.at[layer], q_recv.at[layer])
        own_squares = sq[pl.ds(layer * dpn + dp, 1)][0]
        for o in range(1, dpn):
            own_squares = own_squares + sq_in[layer, o - 1]
        row_scale = lax.rsqrt(jnp.sum(own_squares, axis=1, keepdims=True) / D + norm_eps)

        def project(group):
            await_bytes(part_in.at[layer * GROUPS + group], p_recv.at[layer * GROUPS + group])
            summed = part[pl.ds((layer * GROUPS + group) * dpn + dp, 1)][0].astype(jnp.float32)
            for o in range(1, dpn):
                summed = summed + part_in[layer * GROUPS + group, o - 1].astype(jnp.float32)
            summed = (summed * row_scale[None]).astype(jnp.bfloat16).astype(jnp.float32)
            return [summed[i] for i in range(GROUP)]

        def rotated(rows_in, h):
            one = rows_in[:, h * DK : (h + 1) * DK]
            return one * cosine + pltpu.roll(one, half, 1) * sine

        with stage(f"L{layer}_proj0_read"):
            query, key = project(0)
            queries = [rotated(query, h) for h in range(heads)]
            tall = jnp.concatenate(queries, axis=0)
            tall_row = lax.broadcasted_iota(jnp.int32, tall.shape, 0) % seqs
            wide = jnp.concatenate([jnp.where(tall_row == s, tall, 0.0) for s in range(seqs)], axis=1)
            read = jnp.dot(
                wide.astype(jnp.bfloat16), state_t[layer], preferred_element_type=jnp.float32
            )
            rotated_keys = [rotated(key, h) * DK ** (-0.5) for h in range(heads)]
            scores = [
                jnp.sum(queries[h] * rotated_keys[h], axis=1, keepdims=True) for h in range(heads)
            ]
            gains = head_in[layer : layer + 1, :].astype(jnp.float32)
        with stage(f"L{layer}_proj1_norm"):
            value, gate = project(1)
            silu = gate / (1.0 + jnp.exp(-gate))
            outs = []
            for h in range(heads):
                at = slice(h * DK, (h + 1) * DK)
                readout = read[h * seqs : (h + 1) * seqs, at] + scores[h] * value[:, at]
                mean = jnp.sum(readout, axis=1, keepdims=True) / DK
                square = jnp.sum(readout * readout, axis=1, keepdims=True) / DK
                grouped = (readout - mean) * lax.rsqrt(square - mean * mean + group_eps)
                outs.append(silu[:, at] * grouped * gains[:, at])
            gated[pl.ds(layer * dpn + dp, 1)] = jnp.concatenate(outs, axis=1).astype(jnp.bfloat16)[None]
            for o in reversed(range(1, dpn)):
                send(
                    gated.at[layer * dpn + dp],
                    gated.at[layer * dpn + dp],
                    3,
                    g_recv.at[layer],
                    (tp, dp_peers[o]),
                )

        def advance(first_seq, last_seq):
            for s in range(first_seq, last_seq):
                for h in range(heads):
                    at = slice(h * DK, (h + 1) * DK)
                    new_states[layer, s, at] = (
                        decay_of(h) * state_in[layer, s, at]
                        + turned[at, s : s + 1] * rotated_keys[h][s : s + 1]
                    )

        with stage(f"L{layer}_adv1"):
            turned = jnp.transpose(value)
            advance(0, seqs // 2)
        got_back[layer].wait()
        with stage(f"L{layer}_wait_g"):
            await_bytes(gated.at[pl.ds(layer * dpn, dpn - 1)], g_recv.at[layer])
        with stage(f"L{layer}_outdot"):
            every = gated[layer * dpn : (layer + 1) * dpn].reshape(dpn * seqs, columns)
            product = jnp.dot(every, w_back[layer], preferred_element_type=jnp.float32)
            branch[first : first + tpn] = product.reshape(tpn, rows, features).astype(jnp.bfloat16)
            for o in tp_order:
                send(
                    branch.at[first + tp_peers[o]],
                    branch_in.at[layer, o - 1],
                    4,
                    b_recv.at[layer],
                    (tp_peers[o], dp),
                )
        with stage(f"L{layer}_adv2"):
            advance(seqs // 2, seqs)
            if layer + 1 < LAYERS:
                turn_state(layer + 1)
        with stage(f"L{layer}_wait_b"):
            await_bytes(branch_in.at[layer], b_recv.at[layer])
        added = branch[pl.ds(first + tp, 1)][0].astype(jnp.float32)
        for o in range(1, tpn):
            added = added + branch_in[layer, o - 1].astype(jnp.float32)
        new_x = (x_own + added).astype(jnp.bfloat16)
        if layer + 1 < LAYERS:
            fresh[...] = new_x
            gathered[pl.ds(first + tpn + tp, 1)] = new_x[None]
            x_own = new_x.astype(jnp.float32)
            spread_x(layer + 1, fresh)
        else:
            hidden[...] = new_x
    with stage("wait_sent"):
        await_bytes(gathered.at[pl.ds(0, LAYERS * (tpn - 1))], send_sem.at[0])
        await_bytes(sq.at[pl.ds(0, LAYERS * (dpn - 1))], send_sem.at[1])
        await_bytes(part.at[pl.ds(0, LAYERS * GROUPS * (dpn - 1))], send_sem.at[2])
        await_bytes(gated.at[pl.ds(0, LAYERS * (dpn - 1))], send_sem.at[3])
        await_bytes(branch.at[pl.ds(0, LAYERS * (tpn - 1))], send_sem.at[4])


def deliver_kernel(hidden_in, states_in, hidden, states, sem):
    layers, seqs = states.shape[:2]
    pieces = math.gcd(seqs, OUT_PIECES)
    copies = [pltpu.make_async_copy(hidden_in, hidden, sem.at[0])]
    for piece in range(layers * pieces):
        at = (piece // pieces, pl.ds(piece % pieces * (seqs // pieces), seqs // pieces))
        copies.append(pltpu.make_async_copy(states_in.at[at], states.at[at], sem.at[1]))
    for copy in copies:
        copy.start()
    copies[0].wait()
    await_bytes(states, sem.at[1])


def body(tokens, lengths, states, norm_gain, w_query, w_key, w_value, w_gate, head_gain, w_out):
    columns = w_query.shape[2]
    if columns % DK:
        return split_head_body(
            tokens, lengths, states, norm_gain, w_query, w_key, w_value, w_gate, head_gain, w_out
        )
    tpn, dpn = lax.axis_size("tp"), lax.axis_size("dp")
    rows, features = tokens.shape
    seqs = lengths.shape[0]
    vmem = pl.BlockSpec(memory_space=pltpu.VMEM)
    away = pl.BlockSpec(memory_space=pltpu.HBM)
    dma = pltpu.SemaphoreType.DMA
    bf16, f32 = jnp.bfloat16, jnp.float32
    hidden, new_states = pl.pallas_call(
        step_kernel,
        out_shape=(
            pltpu.VMEM((rows, features), bf16),
            pltpu.VMEM(states.shape, f32),
        ),
        in_specs=[away] * 10,
        out_specs=(vmem, vmem),
        scratch_shapes=[
            pltpu.SMEM(lengths.shape, jnp.int32),
            pltpu.VMEM(norm_gain.shape, bf16),
            pltpu.VMEM(head_gain.shape, bf16),
            pltpu.VMEM((LAYERS, seqs, columns, DK), f32),
            pltpu.VMEM((LAYERS, seqs * DK, columns), bf16),
            pltpu.VMEM((LAYERS, KINDS, features, columns), bf16),
            pltpu.VMEM((LAYERS, columns, features), bf16),
            pltpu.VMEM((LAYERS * tpn, rows, features), bf16),
            pltpu.VMEM((LAYERS * GROUPS * dpn, GROUP, seqs, columns), bf16),
            pltpu.VMEM((LAYERS * GROUPS, dpn - 1, GROUP, seqs, columns), bf16),
            pltpu.VMEM((LAYERS * dpn, seqs, DK), f32),
            pltpu.VMEM((LAYERS, dpn - 1, seqs, DK), f32),
            pltpu.VMEM((LAYERS * dpn, seqs, columns), bf16),
            pltpu.VMEM((LAYERS * tpn, rows, features), bf16),
            pltpu.VMEM((LAYERS, tpn - 1, rows, features), bf16),
            pltpu.VMEM((rows, features), bf16),
            dma((4,)),
            dma((LAYERS,)),
            dma((LAYERS,)),
            dma((LAYERS,)),
            dma((5,)),
            dma((LAYERS,)),
            dma((LAYERS * GROUPS,)),
            dma((LAYERS,)),
            dma((LAYERS,)),
            dma((LAYERS,)),
        ],
        compiler_params=pltpu.CompilerParams(collective_id=0, has_side_effects=True, vmem_limit_bytes=40 * 1024 * 1024),
    )(
        *(
            pltpu.with_memory_space_constraint(a, pltpu.HBM)
            for a in (
                tokens,
                lengths,
                norm_gain,
                head_gain,
                states,
                w_query,
                w_key,
                w_value,
                w_gate,
                w_out,
            )
        )
    )
    return pl.pallas_call(
        deliver_kernel,
        out_shape=(
            jax.ShapeDtypeStruct((rows, features), bf16),
            jax.ShapeDtypeStruct(states.shape, f32),
        ),
        in_specs=[vmem, vmem],
        out_specs=(away, away),
        scratch_shapes=[dma((2,))],
        compiler_params=pltpu.CompilerParams(vmem_limit_bytes=8 * 1024 * 1024),
    )(hidden, new_states)


def solution(mesh):
    placed = (
        P("tp", "dp"),
        P("dp"),
        P(None, "dp", "tp", None),
        P(None, "dp"),
        P(None, "dp", "tp"),
        P(None, "dp", "tp"),
        P(None, "dp", "tp"),
        P(None, "dp", "tp"),
        P(None, "tp"),
        P(None, "tp", "dp"),
    )
    return jax.shard_map(
        body,
        mesh=mesh,
        in_specs=placed,
        out_specs=(P("tp", "dp"), P(None, "dp", "tp", None)),
        check_vma=False,
    )
```

```python
import contextlib
import functools
import math

import jax
import jax.numpy as jnp
from jax import lax
from jax.experimental import pallas as pl
from jax.experimental.pallas import tpu as pltpu
from jax.sharding import PartitionSpec as P

D = 4096
HEADS = 16
DK = 128
LAYERS = 2


norm_eps = 1e-06
group_eps = 1e-05
rotary_base = 10000.0


def partner_2(value, axis, apart):
    mask = 2**apart
    pairs = [(source, source ^ mask) for source in range(lax.axis_size(axis))]
    return lax.ppermute(value, axis, pairs)


def rotate(values, positions):
    half_size = values.shape[-1] // 2
    inverse = rotary_base ** (-jnp.arange(half_size, dtype=jnp.float32) / half_size)
    angles = positions.astype(jnp.float32)[:, None] * inverse[None, :]
    cosine = jnp.cos(angles)[:, None, :]
    sine_v = jnp.sin(angles)[:, None, :]
    first_part = values[..., :half_size]
    second = values[..., half_size:]
    return jnp.concatenate(
        [first_part * cosine - second * sine_v, first_part * sine_v + second * cosine], axis=-1
    )


def decays(head_ids):
    return 1.0 - jnp.exp2(-1.0 - 9.0 * head_ids.astype(jnp.float32) / (HEADS - 1))


def split_head_body(tokens, lengths, states, norm_gain, w_query, w_key, w_value, w_gate, head_gain, w_out):
    tp_index = lax.axis_index("tp")
    dp_index = lax.axis_index("dp")
    tp_count = lax.axis_size("tp")
    columns = w_query.shape[2]
    pieces = max(DK // columns, 1)
    levels = pieces.bit_length() - 1
    local_heads = max(columns // DK, 1)
    value_cols = columns // local_heads
    head_ids = tp_index * columns // DK + jnp.arange(local_heads, dtype=jnp.int32)
    gammas = decays(head_ids)
    hidden_x = tokens
    outputs = []
    for layer_id in range(LAYERS):
        prior_state = states[layer_id]
        row_total = prior_state.shape[0]
        local_rows = hidden_x.shape[0]
        x_float = hidden_x.astype(jnp.float32)
        feature_gain = norm_gain[layer_id].astype(jnp.float32)
        weights = jnp.concatenate(
            [w_query[layer_id], w_key[layer_id], w_value[layer_id], w_gate[layer_id]], axis=1
        )
        gathered = lax.all_gather(hidden_x, "tp", axis=0, tiled=True)
        gathered_f = gathered.astype(jnp.float32)
        normed = (gathered_f * feature_gain).astype(jnp.bfloat16)
        partial_value = jnp.dot(normed, weights, preferred_element_type=jnp.float32)
        squares_full = jnp.zeros((local_rows * tp_count,), jnp.float32)
        squares_full = lax.dynamic_update_slice_in_dim(
            squares_full, jnp.sum(x_float * x_float, axis=1), tp_index * local_rows, 0
        )
        all_squares = lax.psum(squares_full, ("tp", "dp"))
        summed = lax.psum_scatter(partial_value, "dp", scatter_dimension=0, tiled=True)
        own_squares = lax.dynamic_slice_in_dim(all_squares, dp_index * row_total, row_total, 0)
        row_scale = lax.rsqrt(own_squares / D + norm_eps)
        projected = (summed * row_scale[:, None]).astype(jnp.bfloat16)
        query_rows = projected[:, :columns]
        key_rows = projected[:, columns : 2 * columns]
        value_rows = projected[:, 2 * columns : 3 * columns]
        gate_rows = projected[:, 3 * columns :]
        stacked = jnp.stack([query_rows, key_rows])
        for join_level_id in range(levels):
            partner = partner_2(stacked, "tp", join_level_id)
            upper_bit = tp_index // 2**join_level_id % 2
            stacked = jnp.where(
                upper_bit == 1,
                jnp.concatenate([partner, stacked], axis=-1),
                jnp.concatenate([stacked, partner], axis=-1),
            )
        query_f = rotate(
            stacked[0].astype(jnp.float32).reshape(row_total, local_heads, DK), lengths
        )
        key_f = rotate(
            stacked[1].astype(jnp.float32).reshape(row_total, local_heads, DK), lengths
        ) * DK ** (-0.5)
        values_f = value_rows.astype(jnp.float32).reshape(row_total, local_heads, value_cols)
        state_view = prior_state.reshape(row_total, local_heads, value_cols, DK)
        updated = gammas[None, :, None, None] * state_view + jnp.einsum(
            "shd,shv->shvd", key_f, values_f
        )
        readout = jnp.einsum("shd,shvd->shv", query_f, updated)
        head_stats = jnp.stack([jnp.sum(readout, axis=-1), jnp.sum(readout * readout, axis=-1)])
        for level_id in range(levels):
            head_stats = head_stats + partner_2(head_stats, "tp", level_id)
        mean_v = head_stats[0][..., None] / DK
        square = head_stats[1][..., None] / DK
        grouped = ((readout - mean_v) * lax.rsqrt(square - mean_v * mean_v + group_eps)).reshape(
            row_total, columns
        )
        grouped = grouped * head_gain[layer_id].astype(jnp.float32)
        gated_rows = (jax.nn.silu(gate_rows.astype(jnp.float32)) * grouped).astype(jnp.bfloat16)
        out_weight = w_out[layer_id]
        whole_weight = lax.all_gather(out_weight, "tp", axis=0, tiled=True)
        every_row = lax.all_gather(gated_rows, "dp", axis=0, tiled=True)
        owned_rows = lax.all_to_all(every_row, "tp", split_axis=0, concat_axis=1, tiled=True)
        branch = jnp.dot(owned_rows, whole_weight, preferred_element_type=jnp.float32)
        hidden_x, updated = (
            (x_float + branch).astype(jnp.bfloat16),
            updated.reshape(row_total, columns, DK),
        )
        outputs.append(updated)
    return (hidden_x, jnp.stack(outputs))


MESH = pl.DeviceIdType.MESH
KINDS = 4
GROUP = 2
GROUPS = KINDS // GROUP
OUT_PIECES = 4
TRACED = False


def stage(name):
    return jax.named_scope(name) if TRACED else contextlib.nullcontext()


def decay_row(columns):
    channel = lax.axis_index("tp") * columns + lax.broadcasted_iota(jnp.int32, (1, columns), 1)
    head = (channel // DK).astype(jnp.float32)
    return 1.0 - jnp.exp((-1.0 - 9.0 * head / (HEADS - 1)) * math.log(2.0))


def flipped(index, mask):
    for bit in range(mask.bit_length()):
        if mask >> bit & 1:
            index = index + (1 - index // 2**bit % 2 * 2) * 2**bit
    return index


def peers_of(index, count):
    if count & (count - 1):
        return [lax.rem(index + o, count) for o in range(count)]
    return [flipped(index, mask) for mask in range(count)]


def await_bytes(ref, sem):
    pltpu.make_async_copy(ref, ref, sem).wait()


def step_kernel(
    tokens,
    lengths,
    norm_gain,
    head_gain,
    states,
    w_query,
    w_key,
    w_value,
    w_gate,
    w_out,
    hidden,
    new_states,
    length_in,
    norm_in,
    head_in,
    state_in,
    state_t,
    w_in,
    w_back,
    gathered,
    part,
    part_in,
    sq,
    sq_in,
    gated,
    branch,
    branch_in,
    fresh,
    small_sem,
    w_sem,
    state_sem,
    back_sem,
    send_sem,
    x_recv,
    p_recv,
    q_recv,
    g_recv,
    b_recv,
):
    tp, dp = lax.axis_index("tp"), lax.axis_index("dp")
    tpn, dpn = lax.axis_size("tp"), lax.axis_size("dp")
    rows, features = tokens.shape
    seqs, columns = new_states.shape[1:3]
    heads = columns // DK
    total = rows * tpn
    per_block = seqs // rows

    barrier = pltpu.get_barrier_semaphore()
    tp_peers, dp_peers = peers_of(tp, tpn), peers_of(dp, dpn)
    for o in range(1, tpn):
        pl.semaphore_signal(barrier, inc=1, device_id=(tp_peers[o], dp), device_id_type=MESH)
    for o in range(1, dpn):
        pl.semaphore_signal(barrier, inc=1, device_id=(tp, dp_peers[o]), device_id_type=MESH)

    def load(src, dst, sem):
        copy = pltpu.make_async_copy(src, dst, sem)
        copy.start()
        return copy

    got_x = load(tokens, gathered.at[tp], small_sem.at[0])
    got_small = [
        load(lengths, length_in, small_sem.at[1]),
        load(norm_gain, norm_in, small_sem.at[2]),
        load(head_gain, head_in, small_sem.at[3]),
    ]
    for copy in [got_x, *got_small]:
        copy.wait()
    got_state, got_back = [], []
    for layer in range(LAYERS):
        for j, w in enumerate((w_query, w_key, w_value, w_gate)):
            load(w.at[layer], w_in.at[layer, j], w_sem.at[layer])
        got_state.append(load(states.at[layer], state_in.at[layer], state_sem.at[layer]))
        got_back.append(load(w_out.at[layer], w_back.at[layer], back_sem.at[layer]))

    half = DK // 2
    lane = lax.broadcasted_iota(jnp.int32, (seqs, DK), 1)
    row = lax.broadcasted_iota(jnp.int32, (seqs, DK), 0)
    position = jnp.zeros((seqs, DK), jnp.float32)
    for s in range(seqs):
        position = jnp.where(row == s, length_in[s].astype(jnp.float32), position)
    inverse = jnp.exp((lane % half).astype(jnp.float32) * (-math.log(rotary_base) / half))
    angle = position * inverse
    cosine = jnp.cos(angle)
    sine = jnp.sin(angle)
    sine = jnp.where(lane < half, -sine, sine)
    gamma = decay_row(columns)

    def decay_of(h):
        return gamma[:, h * DK : h * DK + 1]

    with stage("bar_wait"):
        pl.semaphore_wait(barrier, tpn + dpn - 2)

    def send(src, dst, kind, recv_sem, where):
        pltpu.make_async_remote_copy(
            src_ref=src,
            dst_ref=dst,
            send_sem=send_sem.at[kind],
            recv_sem=recv_sem,
            device_id=where,
            device_id_type=MESH,
        ).start()

    tp_order = sorted(range(1, tpn), key=lambda o: (-o.bit_count(), -o))

    dp_order = list(range(1, dpn))[::-1]
    last_order = sorted(dp_order, key=lambda o: (o % 2, -o))

    def spread_x(layer, src):
        for o in tp_order:
            send(src, gathered.at[layer * tpn + tp], 0, x_recv.at[layer], (tp_peers[o], dp))

    def turn_state(layer):
        got_state[layer].wait()
        for s in range(seqs):
            block = jnp.transpose(state_in[layer, s])
            state_t[layer, s * DK : (s + 1) * DK] = (block * gamma).astype(jnp.bfloat16)

    spread_x(0, gathered.at[tp])
    x_own = gathered[pl.ds(tp, 1)][0].astype(jnp.float32)
    with stage("turn0"):
        turn_state(0)
    for layer in range(LAYERS):
        first = layer * tpn
        await_bytes(w_in.at[layer], w_sem.at[layer])
        with stage(f"L{layer}_wait_x"):
            await_bytes(gathered.at[pl.ds(first, tpn - 1)], x_recv.at[layer])
        x_all = gathered[first : first + tpn].astype(jnp.float32).reshape(total, features)
        normed = (x_all * norm_in[layer : layer + 1, :].astype(jnp.float32)).astype(jnp.bfloat16)
        for group in range(GROUPS):
            slot = (layer * GROUPS + group) * dpn
            with stage(f"L{layer}_dots{group}"):
                for i in range(GROUP):
                    product = jnp.dot(
                        normed, w_in[layer, group * GROUP + i], preferred_element_type=jnp.float32
                    )
                    part[slot : slot + dpn, i] = product.astype(jnp.bfloat16).reshape(dpn, seqs, columns)
                if group == 0:
                    squares = x_all[:, :DK] * x_all[:, :DK]
                    for at in range(DK, features, DK):
                        squares = squares + x_all[:, at : at + DK] * x_all[:, at : at + DK]
                    squares = jnp.concatenate([squares] * (sq.shape[2] // total), axis=0)
                    sq[layer] = jnp.sum(jnp.transpose(squares), axis=0, keepdims=True)
                if group == 0:
                    for o in dp_order:
                        send(sq.at[layer], sq_in.at[layer, o - 1], 1, q_recv.at[layer], (tp, dp_peers[o]))
                for o in dp_order:
                    send(
                        part.at[slot + dp_peers[o]],
                        part_in.at[layer * GROUPS + group, o - 1],
                        2,
                        p_recv.at[layer * GROUPS + group],
                        (tp, dp_peers[o]),
                    )
        with stage(f"L{layer}_wait_sq"):
            await_bytes(sq_in.at[layer], q_recv.at[layer])
        all_squares = sq[layer]
        for o in range(1, dpn):
            all_squares = all_squares + sq_in[layer, o - 1]
        own = lax.broadcasted_iota(jnp.int32, (seqs, sq.shape[2]), 1) - dp * seqs
        own = own == lax.broadcasted_iota(jnp.int32, (seqs, sq.shape[2]), 0)
        own_squares = jnp.sum(jnp.where(own, all_squares, 0.0), axis=1, keepdims=True)
        row_scale = lax.rsqrt(own_squares / D + norm_eps)

        def project(group):
            await_bytes(part_in.at[layer * GROUPS + group], p_recv.at[layer * GROUPS + group])
            summed = part[pl.ds((layer * GROUPS + group) * dpn + dp, 1)][0].astype(jnp.float32)
            for o in range(1, dpn):
                summed = summed + part_in[layer * GROUPS + group, o - 1].astype(jnp.float32)
            summed = (summed * row_scale[None]).astype(jnp.bfloat16).astype(jnp.float32)
            return [summed[i] for i in range(GROUP)]

        def rotated(rows_in, h):
            one = rows_in[:, h * DK : (h + 1) * DK]
            return one * cosine + pltpu.roll(one, half, 1) * sine

        with stage(f"L{layer}_proj0_read"):
            query, key = project(0)
            queries = [rotated(query, h) for h in range(heads)]
            tall = jnp.concatenate(queries, axis=0)
            tall_row = lax.broadcasted_iota(jnp.int32, tall.shape, 0) % seqs
            wide = jnp.concatenate([jnp.where(tall_row == s, tall, 0.0) for s in range(seqs)], axis=1)
            read = jnp.dot(
                wide.astype(jnp.bfloat16), state_t[layer], preferred_element_type=jnp.float32
            )
            rotated_keys = [rotated(key, h) * DK ** (-0.5) for h in range(heads)]
            scores = [
                jnp.sum(queries[h] * rotated_keys[h], axis=1, keepdims=True) for h in range(heads)
            ]
            gains = head_in[layer : layer + 1, :].astype(jnp.float32)
        with stage(f"L{layer}_proj1_norm"):
            value, gate = project(1)
            silu = gate / (1.0 + jnp.exp(-gate))
            outs = []
            for h in range(heads):
                at = slice(h * DK, (h + 1) * DK)
                readout = read[h * seqs : (h + 1) * seqs, at] + scores[h] * value[:, at]
                mean = jnp.sum(readout, axis=1, keepdims=True) / DK
                square = jnp.sum(readout * readout, axis=1, keepdims=True) / DK
                grouped = (readout - mean) * lax.rsqrt(square - mean * mean + group_eps)
                outs.append(silu[:, at] * grouped * gains[:, at])
            own_rows = jnp.concatenate(outs, axis=1).astype(jnp.bfloat16)
            gated[pl.ds(layer * dpn + dp, 1)] = own_rows[None]
            for o in dp_order:
                send(
                    gated.at[layer * dpn + dp],
                    gated.at[layer * dpn + dp],
                    3,
                    g_recv.at[layer],
                    (tp, dp_peers[o]),
                )

        def advance(first_seq, last_seq):
            for s in range(first_seq, last_seq):
                for h in range(heads):
                    at = slice(h * DK, (h + 1) * DK)
                    new_states[layer, s, at] = (
                        decay_of(h) * state_in[layer, s, at]
                        + turned[at, s : s + 1] * rotated_keys[h][s : s + 1]
                    )

        def send_row(owner):
            send(
                branch.at[first + owner],
                branch_in.at[layer, tp],
                4,
                b_recv.at[layer],
                (owner, dp),
            )

        def project_out(rows_in, blocks):
            product = jnp.dot(rows_in, w_back[layer], preferred_element_type=jnp.float32)
            product = product.astype(jnp.bfloat16).reshape(len(blocks), per_block, rows, features)
            for i, block in enumerate(blocks):
                branch[pl.ds(first + block * per_block, per_block)] = product[i]
            for block in blocks:
                for k in range(per_block):
                    owner = block * per_block + lax.rem(tp + 1 + k, per_block)
                    pl.when(owner != tp)(functools.partial(send_row, owner))

        got_back[layer].wait()
        if layer + 1 == LAYERS:
            with stage(f"L{layer}_own_out"):
                project_out(own_rows, [dp])
        with stage(f"L{layer}_adv1"):
            turned = jnp.transpose(value)
            advance(0, seqs // 2)
        with stage(f"L{layer}_wait_g"):
            await_bytes(gated.at[pl.ds(layer * dpn, dpn - 1)], g_recv.at[layer])
        with stage(f"L{layer}_outdot"):
            if layer + 1 < LAYERS:
                every = gated[layer * dpn : (layer + 1) * dpn].reshape(total, columns)
                product = jnp.dot(every, w_back[layer], preferred_element_type=jnp.float32)
                branch[first : first + tpn] = product.reshape(tpn, rows, features).astype(jnp.bfloat16)
                for o in tp_order:
                    send_row(tp_peers[o])
            else:
                project_out(
                    jnp.concatenate([gated[pl.ds(layer * dpn + dp_peers[o], 1)][0] for o in last_order], axis=0),
                    [dp_peers[o] for o in last_order],
                )
        with stage(f"L{layer}_adv2"):
            advance(seqs // 2, seqs)
        if layer + 1 < LAYERS:
            with stage(f"L{layer}_turn"):
                turn_state(layer + 1)
        with stage(f"L{layer}_wait_b"):
            await_bytes(branch.at[pl.ds(0, tpn - 1)], b_recv.at[layer])
        branch_in[layer, pl.ds(tp, 1)] = branch[pl.ds(first + tp, 1)]
        added = branch_in[layer, 0].astype(jnp.float32)
        for o in range(1, tpn):
            added = added + branch_in[layer, o].astype(jnp.float32)
        new_x = (x_own + added).astype(jnp.bfloat16)
        if layer + 1 < LAYERS:
            fresh[...] = new_x
            gathered[pl.ds(first + tpn + tp, 1)] = new_x[None]
            x_own = new_x.astype(jnp.float32)
            spread_x(layer + 1, fresh)
        else:
            hidden[...] = new_x
    with stage("wait_sent"):
        await_bytes(gathered.at[pl.ds(0, LAYERS * (tpn - 1))], send_sem.at[0])
        await_bytes(sq_in, send_sem.at[1])
        await_bytes(part.at[pl.ds(0, LAYERS * GROUPS * (dpn - 1))], send_sem.at[2])
        await_bytes(gated.at[pl.ds(0, LAYERS * (dpn - 1))], send_sem.at[3])
        await_bytes(branch.at[pl.ds(0, LAYERS * (tpn - 1))], send_sem.at[4])


def deliver_kernel(hidden_in, states_in, hidden, states, sem):
    layers, seqs = states.shape[:2]
    pieces = math.gcd(seqs, OUT_PIECES)
    copies = [pltpu.make_async_copy(hidden_in, hidden, sem.at[0])]
    for piece in range(layers * pieces):
        at = (piece // pieces, pl.ds(piece % pieces * (seqs // pieces), seqs // pieces))
        copies.append(pltpu.make_async_copy(states_in.at[at], states.at[at], sem.at[1]))
    for copy in copies:
        copy.start()
    copies[0].wait()
    await_bytes(states, sem.at[1])


def body(tokens, lengths, states, norm_gain, w_query, w_key, w_value, w_gate, head_gain, w_out):
    columns = w_query.shape[2]
    if columns % DK:
        return split_head_body(
            tokens, lengths, states, norm_gain, w_query, w_key, w_value, w_gate, head_gain, w_out
        )
    tpn, dpn = lax.axis_size("tp"), lax.axis_size("dp")
    rows, features = tokens.shape
    seqs = lengths.shape[0]
    vmem = pl.BlockSpec(memory_space=pltpu.VMEM)
    away = pl.BlockSpec(memory_space=pltpu.HBM)
    dma = pltpu.SemaphoreType.DMA
    bf16, f32 = jnp.bfloat16, jnp.float32
    lanes = rows * tpn * max(DK // (rows * tpn), 1)
    hidden, new_states = pl.pallas_call(
        step_kernel,
        out_shape=(
            pltpu.VMEM((rows, features), bf16),
            pltpu.VMEM(states.shape, f32),
        ),
        in_specs=[away] * 10,
        out_specs=(vmem, vmem),
        scratch_shapes=[
            pltpu.SMEM(lengths.shape, jnp.int32),
            pltpu.VMEM(norm_gain.shape, bf16),
            pltpu.VMEM(head_gain.shape, bf16),
            pltpu.VMEM((LAYERS, seqs, columns, DK), f32),
            pltpu.VMEM((LAYERS, seqs * DK, columns), bf16),
            pltpu.VMEM((LAYERS, KINDS, features, columns), bf16),
            pltpu.VMEM((LAYERS, columns, features), bf16),
            pltpu.VMEM((LAYERS * tpn, rows, features), bf16),
            pltpu.VMEM((LAYERS * GROUPS * dpn, GROUP, seqs, columns), bf16),
            pltpu.VMEM((LAYERS * GROUPS, dpn - 1, GROUP, seqs, columns), bf16),
            pltpu.VMEM((LAYERS, 1, lanes), f32),
            pltpu.VMEM((LAYERS, dpn - 1, 1, lanes), f32),
            pltpu.VMEM((LAYERS * dpn, seqs, columns), bf16),
            pltpu.VMEM((LAYERS * tpn, rows, features), bf16),
            pltpu.VMEM((LAYERS, tpn, rows, features), bf16),
            pltpu.VMEM((rows, features), bf16),
            dma((4,)),
            dma((LAYERS,)),
            dma((LAYERS,)),
            dma((LAYERS,)),
            dma((5,)),
            dma((LAYERS,)),
            dma((LAYERS * GROUPS,)),
            dma((LAYERS,)),
            dma((LAYERS,)),
            dma((LAYERS,)),
        ],
        compiler_params=pltpu.CompilerParams(collective_id=0, has_side_effects=True, vmem_limit_bytes=40 * 1024 * 1024),
    )(
        *(
            pltpu.with_memory_space_constraint(a, pltpu.HBM)
            for a in (
                tokens,
                lengths,
                norm_gain,
                head_gain,
                states,
                w_query,
                w_key,
                w_value,
                w_gate,
                w_out,
            )
        )
    )
    return pl.pallas_call(
        deliver_kernel,
        out_shape=(
            jax.ShapeDtypeStruct((rows, features), bf16),
            jax.ShapeDtypeStruct(states.shape, f32),
        ),
        in_specs=[vmem, vmem],
        out_specs=(away, away),
        scratch_shapes=[dma((2,))],
        compiler_params=pltpu.CompilerParams(vmem_limit_bytes=8 * 1024 * 1024),
    )(hidden, new_states)


def solution(mesh):
    placed = (
        P("tp", "dp"),
        P("dp"),
        P(None, "dp", "tp", None),
        P(None, "dp"),
        P(None, "dp", "tp"),
        P(None, "dp", "tp"),
        P(None, "dp", "tp"),
        P(None, "dp", "tp"),
        P(None, "tp"),
        P(None, "tp", "dp"),
    )
    return jax.shard_map(
        body,
        mesh=mesh,
        in_specs=placed,
        out_specs=(P("tp", "dp"), P(None, "dp", "tp", None)),
        check_vma=False,
    )
```

```python
import contextlib
import functools
import math

import jax
import jax.numpy as jnp
from jax import lax
from jax.experimental import pallas as pl
from jax.experimental.pallas import tpu as pltpu
from jax.sharding import PartitionSpec as P

D = 4096
HEADS = 16
DK = 128
LAYERS = 2


norm_eps = 1e-06
group_eps = 1e-05
rotary_base = 10000.0


def partner_2(value, axis, apart):
    mask = 2**apart
    pairs = [(source, source ^ mask) for source in range(lax.axis_size(axis))]
    return lax.ppermute(value, axis, pairs)


def rotate(values, positions):
    half_size = values.shape[-1] // 2
    inverse = rotary_base ** (-jnp.arange(half_size, dtype=jnp.float32) / half_size)
    angles = positions.astype(jnp.float32)[:, None] * inverse[None, :]
    cosine = jnp.cos(angles)[:, None, :]
    sine_v = jnp.sin(angles)[:, None, :]
    first_part = values[..., :half_size]
    second = values[..., half_size:]
    return jnp.concatenate(
        [first_part * cosine - second * sine_v, first_part * sine_v + second * cosine], axis=-1
    )


def decays(head_ids):
    return 1.0 - jnp.exp2(-1.0 - 9.0 * head_ids.astype(jnp.float32) / (HEADS - 1))


def split_head_body(tokens, lengths, states, norm_gain, w_query, w_key, w_value, w_gate, head_gain, w_out):
    tp_index = lax.axis_index("tp")
    dp_index = lax.axis_index("dp")
    tp_count = lax.axis_size("tp")
    columns = w_query.shape[2]
    pieces = max(DK // columns, 1)
    levels = pieces.bit_length() - 1
    local_heads = max(columns // DK, 1)
    value_cols = columns // local_heads
    head_ids = tp_index * columns // DK + jnp.arange(local_heads, dtype=jnp.int32)
    gammas = decays(head_ids)
    hidden_x = tokens
    outputs = []
    for layer_id in range(LAYERS):
        prior_state = states[layer_id]
        row_total = prior_state.shape[0]
        local_rows = hidden_x.shape[0]
        x_float = hidden_x.astype(jnp.float32)
        feature_gain = norm_gain[layer_id].astype(jnp.float32)
        weights = jnp.concatenate(
            [w_query[layer_id], w_key[layer_id], w_value[layer_id], w_gate[layer_id]], axis=1
        )
        gathered = lax.all_gather(hidden_x, "tp", axis=0, tiled=True)
        gathered_f = gathered.astype(jnp.float32)
        normed = (gathered_f * feature_gain).astype(jnp.bfloat16)
        partial_value = jnp.dot(normed, weights, preferred_element_type=jnp.float32)
        squares_full = jnp.zeros((local_rows * tp_count,), jnp.float32)
        squares_full = lax.dynamic_update_slice_in_dim(
            squares_full, jnp.sum(x_float * x_float, axis=1), tp_index * local_rows, 0
        )
        all_squares = lax.psum(squares_full, ("tp", "dp"))
        summed = lax.psum_scatter(partial_value, "dp", scatter_dimension=0, tiled=True)
        own_squares = lax.dynamic_slice_in_dim(all_squares, dp_index * row_total, row_total, 0)
        row_scale = lax.rsqrt(own_squares / D + norm_eps)
        projected = (summed * row_scale[:, None]).astype(jnp.bfloat16)
        query_rows = projected[:, :columns]
        key_rows = projected[:, columns : 2 * columns]
        value_rows = projected[:, 2 * columns : 3 * columns]
        gate_rows = projected[:, 3 * columns :]
        stacked = jnp.stack([query_rows, key_rows])
        for join_level_id in range(levels):
            partner = partner_2(stacked, "tp", join_level_id)
            upper_bit = tp_index // 2**join_level_id % 2
            stacked = jnp.where(
                upper_bit == 1,
                jnp.concatenate([partner, stacked], axis=-1),
                jnp.concatenate([stacked, partner], axis=-1),
            )
        query_f = rotate(
            stacked[0].astype(jnp.float32).reshape(row_total, local_heads, DK), lengths
        )
        key_f = rotate(
            stacked[1].astype(jnp.float32).reshape(row_total, local_heads, DK), lengths
        ) * DK ** (-0.5)
        values_f = value_rows.astype(jnp.float32).reshape(row_total, local_heads, value_cols)
        state_view = prior_state.reshape(row_total, local_heads, value_cols, DK)
        updated = gammas[None, :, None, None] * state_view + jnp.einsum(
            "shd,shv->shvd", key_f, values_f
        )
        readout = jnp.einsum("shd,shvd->shv", query_f, updated)
        head_stats = jnp.stack([jnp.sum(readout, axis=-1), jnp.sum(readout * readout, axis=-1)])
        for level_id in range(levels):
            head_stats = head_stats + partner_2(head_stats, "tp", level_id)
        mean_v = head_stats[0][..., None] / DK
        square = head_stats[1][..., None] / DK
        grouped = ((readout - mean_v) * lax.rsqrt(square - mean_v * mean_v + group_eps)).reshape(
            row_total, columns
        )
        grouped = grouped * head_gain[layer_id].astype(jnp.float32)
        gated_rows = (jax.nn.silu(gate_rows.astype(jnp.float32)) * grouped).astype(jnp.bfloat16)
        out_weight = w_out[layer_id]
        whole_weight = lax.all_gather(out_weight, "tp", axis=0, tiled=True)
        every_row = lax.all_gather(gated_rows, "dp", axis=0, tiled=True)
        owned_rows = lax.all_to_all(every_row, "tp", split_axis=0, concat_axis=1, tiled=True)
        branch = jnp.dot(owned_rows, whole_weight, preferred_element_type=jnp.float32)
        hidden_x, updated = (
            (x_float + branch).astype(jnp.bfloat16),
            updated.reshape(row_total, columns, DK),
        )
        outputs.append(updated)
    return (hidden_x, jnp.stack(outputs))


MESH = pl.DeviceIdType.MESH
KINDS = 4
GROUP = 2
GROUPS = KINDS // GROUP
OUT_PIECES = 4
TRACED = False


def stage(name):
    return jax.named_scope(name) if TRACED else contextlib.nullcontext()


def decay_row(columns):
    channel = lax.axis_index("tp") * columns + lax.broadcasted_iota(jnp.int32, (1, columns), 1)
    head = (channel // DK).astype(jnp.float32)
    return 1.0 - jnp.exp((-1.0 - 9.0 * head / (HEADS - 1)) * math.log(2.0))


def flipped(index, mask):
    for bit in range(mask.bit_length()):
        if mask >> bit & 1:
            index = index + (1 - index // 2**bit % 2 * 2) * 2**bit
    return index


def peers_of(index, count):
    if count & (count - 1):
        return [lax.rem(index + o, count) for o in range(count)]
    return [flipped(index, mask) for mask in range(count)]


def await_bytes(ref, sem):
    pltpu.make_async_copy(ref, ref, sem).wait()


def step_kernel(
    tokens,
    lengths,
    norm_gain,
    head_gain,
    states,
    w_query,
    w_key,
    w_value,
    w_gate,
    w_out,
    hidden,
    new_states,
    length_in,
    norm_in,
    head_in,
    state_in,
    state_t,
    w_in,
    w_back,
    gathered,
    part,
    part_in,
    sq,
    sq_in,
    gated,
    branch,
    branch_in,
    fresh,
    small_sem,
    w_sem,
    state_sem,
    back_sem,
    send_sem,
    x_recv,
    p_recv,
    q_recv,
    g_recv,
    b_recv,
):
    tp, dp = lax.axis_index("tp"), lax.axis_index("dp")
    tpn, dpn = lax.axis_size("tp"), lax.axis_size("dp")
    rows, features = tokens.shape
    seqs, columns = new_states.shape[1:3]
    heads = columns // DK
    total = rows * tpn
    per_block = seqs // rows

    barrier = pltpu.get_barrier_semaphore()
    tp_peers, dp_peers = peers_of(tp, tpn), peers_of(dp, dpn)
    for o in range(1, tpn):
        pl.semaphore_signal(barrier, inc=1, device_id=(tp_peers[o], dp), device_id_type=MESH)
    for o in range(1, dpn):
        pl.semaphore_signal(barrier, inc=1, device_id=(tp, dp_peers[o]), device_id_type=MESH)

    def load(src, dst, sem):
        copy = pltpu.make_async_copy(src, dst, sem)
        copy.start()
        return copy

    got_x = load(tokens, gathered.at[tp], small_sem.at[0])
    got_small = [
        load(lengths, length_in, small_sem.at[1]),
        load(norm_gain, norm_in, small_sem.at[2]),
        load(head_gain, head_in, small_sem.at[3]),
    ]
    for copy in [got_x, *got_small]:
        copy.wait()
    got_state, got_back = [], []
    for layer in range(LAYERS):
        for j, w in enumerate((w_query, w_key, w_value, w_gate)):
            load(w.at[layer], w_in.at[layer, j], w_sem.at[layer])
        got_state.append(load(states.at[layer], state_in.at[layer], state_sem.at[layer]))
        got_back.append(load(w_out.at[layer], w_back.at[layer], back_sem.at[layer]))

    half = DK // 2
    lane = lax.broadcasted_iota(jnp.int32, (seqs, DK), 1)
    row = lax.broadcasted_iota(jnp.int32, (seqs, DK), 0)
    position = jnp.zeros((seqs, DK), jnp.float32)
    for s in range(seqs):
        position = jnp.where(row == s, length_in[s].astype(jnp.float32), position)
    inverse = jnp.exp((lane % half).astype(jnp.float32) * (-math.log(rotary_base) / half))
    angle = position * inverse
    cosine = jnp.cos(angle)
    sine = jnp.sin(angle)
    sine = jnp.where(lane < half, -sine, sine)
    gamma = decay_row(columns)

    def decay_of(h):
        return gamma[:, h * DK : h * DK + 1]

    with stage("bar_wait"):
        pl.semaphore_wait(barrier, tpn + dpn - 2)

    def send(src, dst, kind, recv_sem, where):
        pltpu.make_async_remote_copy(
            src_ref=src,
            dst_ref=dst,
            send_sem=send_sem.at[kind],
            recv_sem=recv_sem,
            device_id=where,
            device_id_type=MESH,
        ).start()

    tp_order = sorted(range(1, tpn), key=lambda o: (-o.bit_count(), -o))

    dp_order = list(range(1, dpn))[::-1]
    late_blocks = [dp_peers[o] for o in dp_order]
    if dpn & (dpn - 1) == 0 and dpn > 2:
        late_blocks = [dp_peers[o] // 2 * 2 + k for o in range(2, dpn, 2) for k in range(2)]
        late_blocks.append(dp_peers[1])

    def spread_x(layer, src):
        for o in tp_order:
            send(src, gathered.at[layer * tpn + tp], 0, x_recv.at[layer], (tp_peers[o], dp))

    def turn_state(layer):
        got_state[layer].wait()
        for s in range(seqs):
            block = jnp.transpose(state_in[layer, s])
            state_t[layer, s * DK : (s + 1) * DK] = (block * gamma).astype(jnp.bfloat16)

    spread_x(0, gathered.at[tp])
    x_own = gathered[pl.ds(tp, 1)][0].astype(jnp.float32)
    with stage("turn0"):
        turn_state(0)
    for layer in range(LAYERS):
        first = layer * tpn
        await_bytes(w_in.at[layer], w_sem.at[layer])
        with stage(f"L{layer}_wait_x"):
            await_bytes(gathered.at[pl.ds(first, tpn - 1)], x_recv.at[layer])
        x_all = gathered[first : first + tpn].astype(jnp.float32).reshape(total, features)
        normed = (x_all * norm_in[layer : layer + 1, :].astype(jnp.float32)).astype(jnp.bfloat16)
        for group in range(GROUPS):
            slot = (layer * GROUPS + group) * dpn
            with stage(f"L{layer}_dots{group}"):
                for i in range(GROUP):
                    product = jnp.dot(
                        normed, w_in[layer, group * GROUP + i], preferred_element_type=jnp.float32
                    )
                    part[slot : slot + dpn, i] = product.astype(jnp.bfloat16).reshape(dpn, seqs, columns)
                if group == 0:
                    squares = x_all[:, :DK] * x_all[:, :DK]
                    for at in range(DK, features, DK):
                        squares = squares + x_all[:, at : at + DK] * x_all[:, at : at + DK]
                    squares = jnp.concatenate([squares] * (sq.shape[2] // total), axis=0)
                    sq[layer] = jnp.sum(jnp.transpose(squares), axis=0, keepdims=True)
                if group == 0:
                    for o in dp_order:
                        send(sq.at[layer], sq_in.at[layer, o - 1], 1, q_recv.at[layer], (tp, dp_peers[o]))
                for o in dp_order:
                    send(
                        part.at[slot + dp_peers[o]],
                        part_in.at[layer * GROUPS + group, o - 1],
                        2,
                        p_recv.at[layer * GROUPS + group],
                        (tp, dp_peers[o]),
                    )
        with stage(f"L{layer}_wait_sq"):
            await_bytes(sq_in.at[layer], q_recv.at[layer])
        all_squares = sq[layer]
        for o in range(1, dpn):
            all_squares = all_squares + sq_in[layer, o - 1]
        own = lax.broadcasted_iota(jnp.int32, (seqs, sq.shape[2]), 1) - dp * seqs
        own = own == lax.broadcasted_iota(jnp.int32, (seqs, sq.shape[2]), 0)
        own_squares = jnp.sum(jnp.where(own, all_squares, 0.0), axis=1, keepdims=True)
        row_scale = lax.rsqrt(own_squares / D + norm_eps)

        def project(group):
            await_bytes(part_in.at[layer * GROUPS + group], p_recv.at[layer * GROUPS + group])
            summed = part[pl.ds((layer * GROUPS + group) * dpn + dp, 1)][0].astype(jnp.float32)
            for o in range(1, dpn):
                summed = summed + part_in[layer * GROUPS + group, o - 1].astype(jnp.float32)
            summed = (summed * row_scale[None]).astype(jnp.bfloat16).astype(jnp.float32)
            return [summed[i] for i in range(GROUP)]

        def rotated(rows_in, h):
            one = rows_in[:, h * DK : (h + 1) * DK]
            return one * cosine + pltpu.roll(one, half, 1) * sine

        with stage(f"L{layer}_proj0_read"):
            query, key = project(0)
            queries = [rotated(query, h) for h in range(heads)]
            tall = jnp.concatenate(queries, axis=0)
            tall_row = lax.broadcasted_iota(jnp.int32, tall.shape, 0) % seqs
            wide = jnp.concatenate([jnp.where(tall_row == s, tall, 0.0) for s in range(seqs)], axis=1)
            read = jnp.dot(
                wide.astype(jnp.bfloat16), state_t[layer], preferred_element_type=jnp.float32
            )
            rotated_keys = [rotated(key, h) * DK ** (-0.5) for h in range(heads)]
            scores = [
                jnp.sum(queries[h] * rotated_keys[h], axis=1, keepdims=True) for h in range(heads)
            ]
            gains = head_in[layer : layer + 1, :].astype(jnp.float32)
        with stage(f"L{layer}_proj1_norm"):
            value, gate = project(1)
            silu = gate / (1.0 + jnp.exp(-gate))
            outs = []
            for h in range(heads):
                at = slice(h * DK, (h + 1) * DK)
                readout = read[h * seqs : (h + 1) * seqs, at] + scores[h] * value[:, at]
                mean = jnp.sum(readout, axis=1, keepdims=True) / DK
                square = jnp.sum(readout * readout, axis=1, keepdims=True) / DK
                grouped = (readout - mean) * lax.rsqrt(square - mean * mean + group_eps)
                outs.append(silu[:, at] * grouped * gains[:, at])
            own_rows = jnp.concatenate(outs, axis=1).astype(jnp.bfloat16)
            gated[pl.ds(layer * dpn + dp, 1)] = own_rows[None]
            for o in dp_order:
                send(
                    gated.at[layer * dpn + dp],
                    gated.at[layer * dpn + dp],
                    3,
                    g_recv.at[layer],
                    (tp, dp_peers[o]),
                )

        def advance(first_seq, last_seq):
            for s in range(first_seq, last_seq):
                for h in range(heads):
                    at = slice(h * DK, (h + 1) * DK)
                    new_states[layer, s, at] = (
                        decay_of(h) * state_in[layer, s, at]
                        + turned[at, s : s + 1] * rotated_keys[h][s : s + 1]
                    )

        def send_row(owner):
            send(
                branch.at[first + owner],
                branch_in.at[layer, tp],
                4,
                b_recv.at[layer],
                (owner, dp),
            )

        def project_out(rows_in, blocks):
            product = jnp.dot(rows_in, w_back[layer], preferred_element_type=jnp.float32)
            product = product.astype(jnp.bfloat16).reshape(len(blocks), per_block, rows, features)
            for i, block in enumerate(blocks):
                branch[pl.ds(first + block * per_block, per_block)] = product[i]
            for block in blocks:
                for k in range(per_block):
                    owner = block * per_block + lax.rem(tp + 1 + k, per_block)
                    pl.when(owner != tp)(functools.partial(send_row, owner))

        got_back[layer].wait()
        if layer + 1 == LAYERS:
            with stage(f"L{layer}_own_out"):
                project_out(own_rows, [dp])
        with stage(f"L{layer}_adv1"):
            turned = jnp.transpose(value)
            advance(0, seqs // 2)
        with stage(f"L{layer}_wait_g"):
            await_bytes(gated.at[pl.ds(layer * dpn, dpn - 1)], g_recv.at[layer])
        with stage(f"L{layer}_outdot"):
            if layer + 1 < LAYERS:
                every = gated[layer * dpn : (layer + 1) * dpn].reshape(total, columns)
                product = jnp.dot(every, w_back[layer], preferred_element_type=jnp.float32)
                branch[first : first + tpn] = product.reshape(tpn, rows, features).astype(jnp.bfloat16)
                for o in tp_order:
                    send_row(tp_peers[o])
            else:
                late_rows = [gated[pl.ds(layer * dpn + block, 1)][0] for block in late_blocks]
                project_out(jnp.concatenate(late_rows, axis=0), late_blocks)
        with stage(f"L{layer}_adv2"):
            advance(seqs // 2, seqs)
        if layer + 1 < LAYERS:
            with stage(f"L{layer}_turn"):
                turn_state(layer + 1)
        with stage(f"L{layer}_wait_b"):
            await_bytes(branch.at[pl.ds(0, tpn - 1)], b_recv.at[layer])
        branch_in[layer, pl.ds(tp, 1)] = branch[pl.ds(first + tp, 1)]
        added = branch_in[layer, 0].astype(jnp.float32)
        for o in range(1, tpn):
            added = added + branch_in[layer, o].astype(jnp.float32)
        new_x = (x_own + added).astype(jnp.bfloat16)
        if layer + 1 < LAYERS:
            fresh[...] = new_x
            gathered[pl.ds(first + tpn + tp, 1)] = new_x[None]
            x_own = new_x.astype(jnp.float32)
            spread_x(layer + 1, fresh)
        else:
            hidden[...] = new_x
    with stage("wait_sent"):
        await_bytes(gathered.at[pl.ds(0, LAYERS * (tpn - 1))], send_sem.at[0])
        await_bytes(sq_in, send_sem.at[1])
        await_bytes(part.at[pl.ds(0, LAYERS * GROUPS * (dpn - 1))], send_sem.at[2])
        await_bytes(gated.at[pl.ds(0, LAYERS * (dpn - 1))], send_sem.at[3])
        await_bytes(branch.at[pl.ds(0, LAYERS * (tpn - 1))], send_sem.at[4])


def deliver_kernel(hidden_in, states_in, hidden, states, sem):
    layers, seqs = states.shape[:2]
    pieces = math.gcd(seqs, OUT_PIECES)
    copies = [pltpu.make_async_copy(hidden_in, hidden, sem.at[0])]
    for piece in range(layers * pieces):
        at = (piece // pieces, pl.ds(piece % pieces * (seqs // pieces), seqs // pieces))
        copies.append(pltpu.make_async_copy(states_in.at[at], states.at[at], sem.at[1]))
    for copy in copies:
        copy.start()
    copies[0].wait()
    await_bytes(states, sem.at[1])


def body(tokens, lengths, states, norm_gain, w_query, w_key, w_value, w_gate, head_gain, w_out):
    columns = w_query.shape[2]
    if columns % DK:
        return split_head_body(
            tokens, lengths, states, norm_gain, w_query, w_key, w_value, w_gate, head_gain, w_out
        )
    tpn, dpn = lax.axis_size("tp"), lax.axis_size("dp")
    rows, features = tokens.shape
    seqs = lengths.shape[0]
    vmem = pl.BlockSpec(memory_space=pltpu.VMEM)
    away = pl.BlockSpec(memory_space=pltpu.HBM)
    dma = pltpu.SemaphoreType.DMA
    bf16, f32 = jnp.bfloat16, jnp.float32
    lanes = rows * tpn * max(DK // (rows * tpn), 1)
    hidden, new_states = pl.pallas_call(
        step_kernel,
        out_shape=(
            pltpu.VMEM((rows, features), bf16),
            pltpu.VMEM(states.shape, f32),
        ),
        in_specs=[away] * 10,
        out_specs=(vmem, vmem),
        scratch_shapes=[
            pltpu.SMEM(lengths.shape, jnp.int32),
            pltpu.VMEM(norm_gain.shape, bf16),
            pltpu.VMEM(head_gain.shape, bf16),
            pltpu.VMEM((LAYERS, seqs, columns, DK), f32),
            pltpu.VMEM((LAYERS, seqs * DK, columns), bf16),
            pltpu.VMEM((LAYERS, KINDS, features, columns), bf16),
            pltpu.VMEM((LAYERS, columns, features), bf16),
            pltpu.VMEM((LAYERS * tpn, rows, features), bf16),
            pltpu.VMEM((LAYERS * GROUPS * dpn, GROUP, seqs, columns), bf16),
            pltpu.VMEM((LAYERS * GROUPS, dpn - 1, GROUP, seqs, columns), bf16),
            pltpu.VMEM((LAYERS, 1, lanes), f32),
            pltpu.VMEM((LAYERS, dpn - 1, 1, lanes), f32),
            pltpu.VMEM((LAYERS * dpn, seqs, columns), bf16),
            pltpu.VMEM((LAYERS * tpn, rows, features), bf16),
            pltpu.VMEM((LAYERS, tpn, rows, features), bf16),
            pltpu.VMEM((rows, features), bf16),
            dma((4,)),
            dma((LAYERS,)),
            dma((LAYERS,)),
            dma((LAYERS,)),
            dma((5,)),
            dma((LAYERS,)),
            dma((LAYERS * GROUPS,)),
            dma((LAYERS,)),
            dma((LAYERS,)),
            dma((LAYERS,)),
        ],
        compiler_params=pltpu.CompilerParams(collective_id=0, has_side_effects=True, vmem_limit_bytes=40 * 1024 * 1024),
    )(
        *(
            pltpu.with_memory_space_constraint(a, pltpu.HBM)
            for a in (
                tokens,
                lengths,
                norm_gain,
                head_gain,
                states,
                w_query,
                w_key,
                w_value,
                w_gate,
                w_out,
            )
        )
    )
    return pl.pallas_call(
        deliver_kernel,
        out_shape=(
            jax.ShapeDtypeStruct((rows, features), bf16),
            jax.ShapeDtypeStruct(states.shape, f32),
        ),
        in_specs=[vmem, vmem],
        out_specs=(away, away),
        scratch_shapes=[dma((2,))],
        compiler_params=pltpu.CompilerParams(vmem_limit_bytes=8 * 1024 * 1024),
    )(hidden, new_states)


def solution(mesh):
    placed = (
        P("tp", "dp"),
        P("dp"),
        P(None, "dp", "tp", None),
        P(None, "dp"),
        P(None, "dp", "tp"),
        P(None, "dp", "tp"),
        P(None, "dp", "tp"),
        P(None, "dp", "tp"),
        P(None, "tp"),
        P(None, "tp", "dp"),
    )
    return jax.shard_map(
        body,
        mesh=mesh,
        in_specs=placed,
        out_specs=(P("tp", "dp"), P(None, "dp", "tp", None)),
        check_vma=False,
    )
```
